32 devices in a mesh: grp: 2 (over y), st: 4 (over z), tp: 4 (over x, core).
Axes of the slice: x: 2, y: 2, z: 4, core: 2. Of those that a mesh axis runs over, the one named last changes fastest.
Arguments:
- tokens: bfloat16 [8192, 2048], P(('grp', 'st'), 'tp'), parts along dimension 0, may hold values from -6 to 6
- norm_gain: float32 [2048], replicated, may hold values from 0.1 to 1.9
- pool_weight: bfloat16 [4, 512, 512], P('tp'), may hold values from -0.25 to 0.25
- pool_scale: float32 [2048], P('tp'), may hold values from 0.1 to 1.9
- query_weight: bfloat16 [2048, 1024], P(None, 'tp'), may hold values from -3 to 3
- gate_weight: bfloat16 [2048, 8], replicated, may hold values from -0.125 to 0.125
- key_weight: bfloat16 [2048, 1024], P(None, 'tp'), may hold values from -0.125 to 0.125
- value_weight: bfloat16 [2048, 1024], P(None, 'tp'), may hold values from -0.125 to 0.125
- out_weight: bfloat16 [1024, 2048], P(None, 'tp'), may hold values from -0.1875 to 0.1875
- passage_gain: float32 [2048], replicated, may hold values from 0.1 to 1.9
- passage_store: bfloat16 [192, 64, 2048], P(('grp', 'st')), parts along dimension 0, may hold values from -6 to 6
- passage_ids: int32 [64, 4], P(('grp', 'st')), parts along dimension 0, may hold values from 0 to 95, as said below
Outputs:
- mixed: bfloat16 [8192, 2048], P(('grp', 'st'), 'tp'), parts along dimension 0
The draws below stay inside these ranges and needn't reach their ends.
There are 2 independent parts, one for each index of `grp`. The reference program is written for one: setup_inputs(seed, part) draws one part's arguments, and reference() takes and returns one part's arrays. A program takes and returns all parts, laid end to end along the dimension named above; an argument that names none is the same for every part. Nothing has to cross between parts.
Inputs may be any that keep to these rules, and one draw needn't show every extreme that they name: `passage_ids`: the ids of the blocks of one index of st name at most 8 passages held by any one index of st, and exactly 8 held by some index.
All inputs are finite; a program needn't handle non-finite values.
Results may differ from the reference program's by a relative error of at most 0.009.
Values may be sent and summed in bfloat16 or wider, within the bound.
A program may use at most 128 MiB of HBM per device.

```python
import jax
import jax.numpy as jnp
from jax import lax

D = 2048
HEADS = 8
HD = 128
GROUPS = 4
GROUP_CH = 512
SEQ_LEN = 256
BLK = 128
NPB = 4
PLEN = 64
P_DEV = 24
TOKENS = 4096
BLK_DEV = 8
BLOCKS = 32
REQ = 32
CAP = 8
PASSAGES = 96
N_ST = 4


def draw_passage_ids(key, part):
    base_key = jax.random.fold_in(key, 11)
    slots_all = N_ST * CAP
    tickets = jnp.arange(slots_all, dtype=jnp.int32)
    ticket_owner = tickets // CAP

    def one_reader(reader_key, reader):
        order_key, full_key, shuffle_key, first_key, second_key = jax.random.split(reader_key, 5)
        base_rank = jax.random.permutation(order_key, slots_all).astype(jnp.int32)
        full_owner = jax.random.randint(full_key, (), 0, N_ST, dtype=jnp.int32)
        before = (reader + N_ST - 1) % N_ST
        halfway = (reader + N_ST // 2) % N_ST
        forced = (tickets == before * CAP) | (tickets == halfway * CAP)
        ranking = base_rank - 3 * slots_all * (ticket_owner == full_owner).astype(jnp.int32) - slots_all * forced.astype(jnp.int32)
        chosen = jnp.argsort(ranking, stable=True)[:REQ]
        owners = ticket_owner[chosen]
        owners = owners[jax.random.permutation(shuffle_key, REQ)]
        local_index = jnp.minimum(jax.random.randint(first_key, (REQ,), 0, P_DEV, dtype=jnp.int32), jax.random.randint(second_key, (REQ,), 0, P_DEV, dtype=jnp.int32))
        return (owners * P_DEV + local_index).reshape(BLK_DEV, NPB)
    reader_keys = jax.random.split(base_key, N_ST)
    readers = jnp.arange(N_ST, dtype=jnp.int32)
    return jax.vmap(one_reader)(reader_keys, readers).reshape(BLOCKS, NPB).astype(jnp.int32)


def draw_query_weight(key, part):
    base_key = jax.random.fold_in(key, 23)
    normal_key = jax.random.fold_in(base_key, 0)
    weights = jax.random.normal(normal_key, (D, HEADS * HD), jnp.float32) * D ** (-0.5)
    return jnp.clip(weights, -3.0, 3.0).astype(jnp.bfloat16)


def shard_levels(stream_key, shape, shards, least, largest):
    level = 1.0
    for dim, parts in shards:
        draws = jax.random.uniform(jax.random.fold_in(jax.random.fold_in(stream_key, 6), dim), (parts,), jnp.float32, least / len(shards), largest / len(shards))
        level = level * jnp.repeat(jnp.exp(draws), shape[dim] // parts).reshape((-1,) + (1,) * (len(shape) - 1 - dim))
    return level


def gaussian(own_key, shape, spread, bound, cuts=(), kind=jnp.bfloat16):
    factor_of = shard_levels(own_key, shape, cuts, -0.22, 0.18) if cuts else 1.0
    values = jax.random.normal(own_key, shape, jnp.float32) * spread * factor_of
    return jnp.minimum(jnp.maximum(values, -bound), bound).astype(kind)


def setup_inputs(seed: int = 0, part: int = 0) -> dict:
    arg_keys = jax.random.split(jax.random.key(seed), 13)
    part_splits = jax.random.split(jax.random.fold_in(arg_keys[12], part), 13)
    tokens = gaussian(part_splits[0], (TOKENS, D), 1.0, 6.0, ((0, 4), (1, 4)))
    norm_gain = jnp.clip(1.0 + 0.18 * jax.random.normal(arg_keys[1], (D,), jnp.float32), 0.1, 1.9)
    pool_weight = gaussian(arg_keys[2], (GROUPS, GROUP_CH, GROUP_CH), GROUP_CH ** -0.5, 0.25, ((0, 4),))
    pool_scale = jnp.clip(1.0 + 0.18 * jax.random.normal(arg_keys[3], (D,), jnp.float32), 0.1, 1.9)
    query_weight = draw_query_weight(jax.random.fold_in(arg_keys[12], 71), part)
    gate_weight = gaussian(arg_keys[5], (D, HEADS), D ** -0.5, 0.125)
    key_weight = gaussian(arg_keys[6], (D, HEADS * HD), D ** -0.5, 0.125, ((1, 4),))
    value_weight = gaussian(arg_keys[7], (D, HEADS * HD), D ** -0.5, 0.125, ((1, 4),))
    out_weight = gaussian(arg_keys[8], (HEADS * HD, D), (HEADS * HD) ** -0.5, 0.1875, ((1, 4),))
    passage_gain = jnp.clip(1.0 + 0.18 * jax.random.normal(arg_keys[9], (D,), jnp.float32), 0.1, 1.9)
    passage_store = gaussian(part_splits[10], (PASSAGES, PLEN, D), 1.0, 6.0, ((0, 4),))
    passage_ids = draw_passage_ids(jax.random.fold_in(jax.random.fold_in(arg_keys[12], part), 71), part)
    return {"tokens": tokens, "norm_gain": norm_gain, "pool_weight": pool_weight, "pool_scale": pool_scale, "query_weight": query_weight, "gate_weight": gate_weight, "key_weight": key_weight, "value_weight": value_weight, "out_weight": out_weight, "passage_gain": passage_gain, "passage_store": passage_store, "passage_ids": passage_ids}


epsilon = 1e-06

def rms_norm(values, gain):
    wide_values = values.astype(jnp.float32)
    inverse = lax.rsqrt(lax.optimization_barrier(jnp.mean(wide_values * wide_values, axis=-1, keepdims=True)) + epsilon)
    return (wide_values * inverse * gain).astype(jnp.bfloat16)

def reference(tokens, norm_gain, pool_weight, pool_scale, query_weight, gate_weight, key_weight, value_weight, out_weight, passage_gain, passage_store, passage_ids):
    normed = rms_norm(tokens, norm_gain)
    sequences = TOKENS // SEQ_LEN
    channels = D // GROUPS
    grouped = normed.astype(jnp.float32).reshape(sequences, SEQ_LEN, GROUPS, channels)
    running = jnp.cumsum(grouped, axis=1)
    position = jnp.arange(SEQ_LEN)
    pieces = []
    for group_index in range(GROUPS):
        window = 2 ** (group_index + 1)
        current = running[:, :, group_index]
        lagged = jnp.pad(current, ((0, 0), (window, 0), (0, 0)))[:, :SEQ_LEN]
        divisor = jnp.minimum(position + 1, window).astype(jnp.float32)[None, :, None]
        pieces.append((current - lagged) / divisor - grouped[:, :, group_index])
    pooled = jnp.stack(pieces, axis=2).astype(jnp.bfloat16).reshape(TOKENS, GROUPS, channels)
    mixing = jnp.einsum('tgc,gcd->tgd', pooled.astype(jnp.float32), pool_weight.astype(jnp.float32)).reshape(TOKENS, D) * pool_scale
    queries = jnp.dot(normed, query_weight, preferred_element_type=jnp.float32).astype(jnp.bfloat16)
    gating = jax.nn.sigmoid(jnp.dot(normed, gate_weight, preferred_element_type=jnp.float32))
    query_blocks = queries.reshape(BLOCKS, BLK, HEADS, HD)
    gate_blocks = gating.reshape(BLOCKS, BLK, HEADS)

    def one_block(inputs):
        block_queries, block_gates, block_ids = inputs
        fetched = jnp.take(passage_store, block_ids, axis=0).reshape(NPB * PLEN, D)
        passage_rows = rms_norm(fetched, passage_gain)
        key_rows = jnp.dot(passage_rows, key_weight, preferred_element_type=jnp.float32).astype(jnp.bfloat16).reshape(NPB * PLEN, HEADS, HD)
        values = jnp.dot(passage_rows, value_weight, preferred_element_type=jnp.float32).astype(jnp.bfloat16).reshape(NPB * PLEN, HEADS, HD)
        scores = jnp.einsum('qhd,khd->hqk', block_queries.astype(jnp.float32), key_rows.astype(jnp.float32)) * HD ** (-0.5)
        row_max = lax.optimization_barrier(jnp.max(scores, axis=-1, keepdims=True))
        weights = jnp.exp(scores - row_max)
        probabilities = (weights / lax.optimization_barrier(jnp.sum(weights, axis=-1, keepdims=True))).astype(jnp.bfloat16)
        attended = jnp.einsum('hqk,khd->qhd', probabilities.astype(jnp.float32), values.astype(jnp.float32))
        return (attended * block_gates[:, :, None]).astype(jnp.bfloat16).reshape(BLK, HEADS * HD)
    head_out = lax.map(one_block, (query_blocks, gate_blocks, passage_ids)).reshape(TOKENS, HEADS * HD)
    crossed = jnp.dot(head_out, out_weight, preferred_element_type=jnp.float32)
    return (mixing + crossed).astype(jnp.bfloat16)
```

```python
import functools

import jax
import jax.numpy as jnp
from jax import lax
from jax.experimental import pallas as pl
from jax.experimental.pallas import tpu as pltpu
from jax.sharding import PartitionSpec as P

HD = 128
SEQ_LEN = 256
BLK = 128
NPB = 4
MESH = pl.DeviceIdType.MESH

epsilon = 1e-06


def flip(index, mask):
    out = index
    bit = 1
    while bit <= mask:
        if mask & bit:
            out = out + bit - 2 * bit * ((index // bit) % 2)
        bit *= 2
    return out


def mixer_kernel(
    n_st,
    n_tp,
    cap,
    asked_ref,
    place_ref,
    tokens_hbm,
    norm_gain_ref,
    pool_weight_hbm,
    pool_scale_ref,
    query_weight_hbm,
    gate_weight_ref,
    key_weight_hbm,
    value_weight_hbm,
    out_weight_hbm,
    passage_gain_ref,
    store_hbm,
    out_ref,
    store,
    wk,
    wv,
    wq,
    wo,
    wp,
    tok,
    kv,
    send,
    recv,
    queries,
    gates,
    total,
    heads_all,
    load_sem,
    store_sem,
    own_sem,
    tok_far_send,
    tok_far_recv,
    tok_sib_send,
    tok_sib_recv,
    tok_fwd_send,
    tok_fwd_recv,
    kv_send,
    kv_recv,
    ho_far_send,
    ho_far_recv,
    ho_sib_send,
    ho_sib_recv,
    ho_fwd_send,
    ho_fwd_recv,
):
    st = lax.axis_index("st")
    tp = lax.axis_index("tp")
    rows = tokens_hbm.shape[0]
    width = tokens_hbm.shape[1]
    full = width * n_tp
    n_head = queries.shape[0]
    n_pass, plen = kv.shape[1], kv.shape[2]
    chunks = rows // SEQ_LEN
    fars = list(range(2, n_tp, 2))
    st_masks = list(range(n_st - 1, 0, -1))
    sib = flip(tp, 1)

    loads = [
        pltpu.make_async_copy(src, dst, load_sem.at[i])
        for i, (src, dst) in enumerate(
            [
                (key_weight_hbm, wk),
                (value_weight_hbm, wv),
                (query_weight_hbm, wq),
                (out_weight_hbm, wo),
                (pool_weight_hbm.at[0], wp),
            ]
        )
    ]
    per_step = SEQ_LEN // plen
    steps = n_pass // per_step

    def store_load(i):
        part = pl.ds(i * per_step, per_step)
        return pltpu.make_async_copy(store_hbm.at[part], store.at[part], store_sem.at[i])

    loads[0].start()
    store_load(0).start()
    loads[1].start()
    for i in range(1, steps):
        store_load(i).start()
    own_load = pltpu.make_async_copy(tokens_hbm, tok.at[tp], own_sem)
    own_load.start()
    for load in loads[2:]:
        load.start()

    barrier = pltpu.get_barrier_semaphore()
    peers = [{"tp": sib}] + [{"tp": flip(tp, m)} for m in fars]
    peers += [{"st": flip(st, m)} for m in st_masks]
    for peer in peers:
        pl.semaphore_signal(barrier, inc=1, device_id=peer, device_id_type=MESH)
    pl.semaphore_wait(barrier, len(peers))

    def remote(src, dst, send_sem, recv_sem, peer):
        return pltpu.make_async_remote_copy(
            src_ref=src,
            dst_ref=dst,
            send_sem=send_sem,
            recv_sem=recv_sem,
            device_id=peer,
            device_id_type=MESH,
        )

    def chunk_rows(r):
        return pl.ds(pl.multiple_of(r * SEQ_LEN, SEQ_LEN), SEQ_LEN)

    def tok_far(i, r):
        return remote(
            tokens_hbm.at[chunk_rows(r)],
            tok.at[tp, chunk_rows(r)],
            tok_far_send.at[i, r],
            tok_far_recv.at[i, r],
            {"tp": flip(tp, fars[i])},
        )

    def tok_sib(r):
        return remote(
            tokens_hbm.at[chunk_rows(r)],
            tok.at[tp, chunk_rows(r)],
            tok_sib_send.at[r],
            tok_sib_recv.at[r],
            {"tp": sib},
        )

    def tok_fwd(i, r):
        ref = tok.at[flip(tp, fars[i]), chunk_rows(r)]
        return remote(ref, ref, tok_fwd_send.at[i, r], tok_fwd_recv.at[i, r], {"tp": sib})

    for r in range(chunks):
        for i in range(len(fars)):
            tok_far(i, r).start()
    for r in range(chunks):
        tok_sib(r).start()

    loads[0].wait()
    loads[1].wait()

    def project(i, carry):
        store_load(i).wait()
        x = store[pl.ds(i * per_step, per_step)].reshape(SEQ_LEN, full)
        wide = x.astype(jnp.float32)
        inverse = lax.rsqrt(jnp.sum(wide * wide, axis=1, keepdims=True) / full + epsilon)
        normed = (wide * inverse * passage_gain_ref[...]).astype(jnp.bfloat16)
        k = jnp.dot(normed, wk[...], preferred_element_type=jnp.float32).astype(jnp.bfloat16)
        v = jnp.dot(normed, wv[...], preferred_element_type=jnp.float32).astype(jnp.bfloat16)
        part = pl.ds(i * per_step, per_step)
        for h in range(n_head):
            cols = slice(h * HD, (h + 1) * HD)
            kv[h, part, :, 0:HD] = k[:, cols].reshape(per_step, plen, HD)
            kv[h, part, :, HD : 2 * HD] = v[:, cols].reshape(per_step, plen, HD)
        return carry

    lax.fori_loop(0, steps, project, 0)

    def kv_copy(h, j):
        return remote(
            send.at[h, j],
            recv[h].at[pl.ds(st * cap, cap)],
            kv_send.at[h, j],
            kv_recv.at[h, j],
            {"st": flip(st, st_masks[j])},
        )

    for h in range(n_head):
        for j, mask in enumerate(st_masks):
            peer = flip(st, mask)
            for c in range(cap):
                send[h, j, c] = kv[h, asked_ref[peer, c]]
            kv_copy(h, j).start()
    for h in range(n_head):
        for c in range(cap):
            recv[h][st * cap + c] = kv[h, asked_ref[st, c]]

    own_load.wait()
    for load in loads[2:]:
        load.wait()
    window_step = tp

    def token_step(r, carry):
        for i in range(len(fars)):
            tok_far(i, r).wait_recv()
            tok_fwd(i, r).start()
        tok_sib(r).wait_recv()
        for i in range(len(fars)):
            tok_fwd(i, r).wait_recv()
        here = chunk_rows(r)
        squares = jnp.zeros((SEQ_LEN, 1), jnp.float32)
        for j in range(n_tp):
            wide = tok[j, here, :].astype(jnp.float32)
            squares = squares + jnp.sum(wide * wide, axis=1, keepdims=True)
        inverse = lax.rsqrt(squares / full + epsilon)
        query = jnp.zeros((SEQ_LEN, n_head * HD), jnp.float32)
        gate = jnp.zeros((SEQ_LEN, gate_weight_ref.shape[1]), jnp.float32)
        for j in range(n_tp):
            cols = pl.ds(j * width, width)
            wide = tok[j, here, :].astype(jnp.float32)
            normed = (wide * inverse * norm_gain_ref[:, cols]).astype(jnp.bfloat16)
            query = query + jnp.dot(normed, wq[cols, :], preferred_element_type=jnp.float32)
            gate = gate + jnp.dot(
                normed, gate_weight_ref[cols, :], preferred_element_type=jnp.float32
            )
        query = query.astype(jnp.bfloat16)
        gate = jax.nn.sigmoid(gate)
        lane = lax.broadcasted_iota(jnp.int32, gate.shape, 1)
        for h in range(n_head):
            queries[h, here, :] = query[:, h * HD : (h + 1) * HD]
            column = jnp.sum(
                jnp.where(lane == tp * n_head + h, gate, 0.0), axis=1, keepdims=True
            )
            gates[h, here, :] = jnp.broadcast_to(column, (SEQ_LEN, HD))
        own_cols = pl.ds(pl.multiple_of(tp * width, width), width)
        wide = tok[tp, here, :].astype(jnp.float32)
        mine = (wide * inverse * norm_gain_ref[:, own_cols]).astype(jnp.bfloat16)
        mine = mine.astype(jnp.float32)
        position = lax.broadcasted_iota(jnp.int32, (SEQ_LEN, width), 0)
        summed = mine
        for level in range(n_tp):
            shift = 2**level
            moved = jnp.where(position >= shift, pltpu.roll(summed, shift, axis=0), 0.0)
            summed = jnp.where(window_step >= level, summed + moved, summed)
        window = jnp.int32(2)
        for level in range(1, n_tp):
            window = jnp.where(window_step >= level, jnp.int32(2 ** (level + 1)), window)
        divisor = jnp.minimum(position + 1, window).astype(jnp.float32)
        pooled = (summed / divisor - mine).astype(jnp.bfloat16)
        mixing = jnp.dot(pooled, wp[...], preferred_element_type=jnp.float32)
        total[here, :] = mixing * pool_scale_ref[...]
        return carry

    lax.fori_loop(0, chunks, token_step, 0)

    def ho_far(h, i, r):
        ref = heads_all.at[h, tp, chunk_rows(r)]
        return remote(
            ref,
            ref,
            ho_far_send.at[h, i, r],
            ho_far_recv.at[h, i, r],
            {"tp": flip(tp, fars[i])},
        )

    def ho_sib(h, r):
        ref = heads_all.at[h, tp, chunk_rows(r)]
        return remote(ref, ref, ho_sib_send.at[h, r], ho_sib_recv.at[h, r], {"tp": sib})

    def ho_fwd(h, i, r):
        ref = heads_all.at[h, flip(tp, fars[i]), chunk_rows(r)]
        return remote(
            ref, ref, ho_fwd_send.at[h, i, r], ho_fwd_recv.at[h, i, r], {"tp": sib}
        )

    blocks = SEQ_LEN // BLK
    scale = HD ** (-0.5)

    for h in range(n_head):
        for j in range(len(st_masks)):
            kv_copy(h, j).wait_recv()

        def attend(r, carry, h=h):
            for inner in range(blocks):
                block = r * blocks + inner
                here = pl.ds(pl.multiple_of(block * BLK, BLK), BLK)
                pieces = [recv[h][place_ref[block * NPB + n]] for n in range(NPB)]
                keys = jnp.concatenate([p[:, :HD] for p in pieces], axis=0)
                vals = jnp.concatenate([p[:, HD:] for p in pieces], axis=0)
                scores = (
                    lax.dot_general(
                        queries[h, here, :],
                        keys,
                        (((1,), (1,)), ((), ())),
                        preferred_element_type=jnp.float32,
                    )
                    * scale
                )
                weights = jnp.exp(scores - jnp.max(scores, axis=1, keepdims=True))
                probs = weights / jnp.sum(weights, axis=1, keepdims=True)
                attended = jnp.dot(
                    probs.astype(jnp.bfloat16), vals, preferred_element_type=jnp.float32
                )
                heads_all[h, tp, here, :] = (attended * gates[h, here, :]).astype(jnp.bfloat16)
            for i in range(len(fars)):
                ho_far(h, i, r).start()
            ho_sib(h, r).start()
            return carry

        lax.fori_loop(0, chunks, attend, 0)

        def forward(r, carry, h=h):
            for i in range(len(fars)):
                ho_far(h, i, r).wait_recv()
                ho_fwd(h, i, r).start()
            return carry

        def finish(r, carry, h=h):
            ho_sib(h, r).wait_recv()
            for i in range(len(fars)):
                ho_fwd(h, i, r).wait_recv()
            here = chunk_rows(r)
            acc = total[here, :]
            for j in range(n_tp):
                acc = acc + jnp.dot(
                    heads_all[h, j, here, :],
                    wo[pl.ds((j * n_head + h) * HD, HD), :],
                    preferred_element_type=jnp.float32,
                )
            if h == n_head - 1:
                out_ref[here, :] = acc.astype(out_ref.dtype)
            else:
                total[here, :] = acc
            return carry

        lax.fori_loop(0, chunks, forward, 0)
        lax.fori_loop(0, chunks, finish, 0)

    def drain(r, carry):
        for i in range(len(fars)):
            tok_far(i, r).wait_send()
            tok_fwd(i, r).wait_send()
        tok_sib(r).wait_send()
        for h in range(n_head):
            for i in range(len(fars)):
                ho_far(h, i, r).wait_send()
                ho_fwd(h, i, r).wait_send()
            ho_sib(h, r).wait_send()
        return carry

    lax.fori_loop(0, chunks, drain, 0)
    for h in range(n_head):
        for j in range(len(st_masks)):
            kv_copy(h, j).wait_send()


def per_device(
    tokens,
    norm_gain,
    pool_weight,
    pool_scale,
    query_weight,
    gate_weight,
    key_weight,
    value_weight,
    out_weight,
    passage_gain,
    passage_store,
    passage_ids,
):
    n_st = lax.axis_size("st")
    n_tp = lax.axis_size("tp")
    rows, width = tokens.shape
    full = width * n_tp
    n_head = query_weight.shape[1] // HD
    n_pass, plen = passage_store.shape[:2]
    chunks = rows // SEQ_LEN
    nf = max(1, (n_tp - 1) // 2)

    flat_ids = passage_ids.reshape(-1)
    asked_count = flat_ids.shape[0]
    cap = max(2, (asked_count + n_st - 1) // n_st)
    owners = flat_ids // n_pass
    local_index = flat_ids % n_pass
    order_index = jnp.arange(asked_count, dtype=jnp.int32)
    earlier = (owners[None, :] == owners[:, None]) & (order_index[None, :] < order_index[:, None])
    slot_index = jnp.sum(earlier.astype(jnp.int32), axis=1)
    place = owners * cap + slot_index
    slot_range = jnp.arange(n_st * cap, dtype=jnp.int32)
    table = jnp.sum(
        jnp.where(place[None, :] == slot_range[:, None], local_index[None, :], 0), axis=1
    ).reshape(n_st, cap)
    asked = lax.all_to_all(table, "st", split_axis=0, concat_axis=0, tiled=True)

    any_spec = pl.BlockSpec(memory_space=pl.ANY)
    vmem = pl.BlockSpec(memory_space=pltpu.VMEM)
    smem = pl.BlockSpec(memory_space=pltpu.SMEM)
    bf = jnp.bfloat16
    dma = pltpu.SemaphoreType.DMA
    return pl.pallas_call(
        functools.partial(mixer_kernel, n_st, n_tp, cap),
        out_shape=jax.ShapeDtypeStruct((rows, width), bf),
        in_specs=[
            smem,
            smem,
            any_spec,
            vmem,
            any_spec,
            vmem,
            any_spec,
            vmem,
            any_spec,
            any_spec,
            any_spec,
            vmem,
            any_spec,
        ],
        out_specs=vmem,
        scratch_shapes=[
            pltpu.VMEM(passage_store.shape, bf),
            pltpu.VMEM(key_weight.shape, bf),
            pltpu.VMEM(value_weight.shape, bf),
            pltpu.VMEM(query_weight.shape, bf),
            pltpu.VMEM(out_weight.shape, bf),
            pltpu.VMEM(pool_weight.shape[1:], bf),
            pltpu.VMEM((n_tp, rows, width), bf),
            pltpu.VMEM((n_head, n_pass, plen, 2 * HD), bf),
            pltpu.VMEM((n_head, n_st - 1, cap, plen, 2 * HD), bf),
            [pltpu.VMEM((n_st * cap, plen, 2 * HD), bf) for _ in range(n_head)],
            pltpu.VMEM((n_head, rows, HD), bf),
            pltpu.VMEM((n_head, rows, HD), jnp.float32),
            pltpu.VMEM((rows, width), jnp.float32),
            pltpu.VMEM((n_head, n_tp, rows, HD), bf),
            dma((5,)),
            dma((n_pass * plen // SEQ_LEN,)),
            dma,
            dma((nf, chunks)),
            dma((nf, chunks)),
            dma((chunks,)),
            dma((chunks,)),
            dma((nf, chunks)),
            dma((nf, chunks)),
            dma((n_head, n_st - 1)),
            dma((n_head, n_st - 1)),
            dma((n_head, nf, chunks)),
            dma((n_head, nf, chunks)),
            dma((n_head, chunks)),
            dma((n_head, chunks)),
            dma((n_head, nf, chunks)),
            dma((n_head, nf, chunks)),
        ],
        compiler_params=pltpu.CompilerParams(
            collective_id=0, has_side_effects=True, vmem_limit_bytes=60 * 1024 * 1024
        ),
        name="mixer",
    )(
        asked,
        place,
        tokens,
        norm_gain.reshape(1, full),
        pool_weight,
        pool_scale.reshape(1, width),
        query_weight,
        gate_weight,
        key_weight,
        value_weight,
        out_weight,
        passage_gain.reshape(1, full),
        passage_store,
    )


def solution(mesh):
    in_specs = (
        P(("grp", "st"), "tp"),
        P(),
        P("tp", None, None),
        P("tp"),
        P(None, "tp"),
        P(),
        P(None, "tp"),
        P(None, "tp"),
        P(None, "tp"),
        P(),
        P(("grp", "st"), None, None),
        P(("grp", "st"), None),
    )
    out_specs = P(("grp", "st"), "tp")
    return jax.shard_map(
        per_device, mesh=mesh, in_specs=in_specs, out_specs=out_specs, check_vma=False
    )
```

```python
import functools

import jax
import jax.numpy as jnp
from jax import lax
from jax.experimental import pallas as pl
from jax.experimental.pallas import tpu as pltpu
from jax.sharding import PartitionSpec as P

HD = 128
SEQ_LEN = 256
BLK = 128
NPB = 4
LANES = 128
MESH = pl.DeviceIdType.MESH

epsilon = 1e-06


def flip(index, mask):
    out = index
    bit = 1
    while bit <= mask:
        if mask & bit:
            out = out + bit - 2 * bit * ((index // bit) % 2)
        bit *= 2
    return out


def mixer_kernel(
    n_st,
    n_tp,
    cap,
    table_ref,
    place_ref,
    tokens_hbm,
    norm_gain_ref,
    pool_weight_hbm,
    pool_scale_ref,
    query_weight_hbm,
    gate_weight_ref,
    key_weight_hbm,
    value_weight_hbm,
    out_weight_hbm,
    passage_gain_ref,
    store_hbm,
    out_ref,
    asked_in,
    asked,
    store,
    wkv,
    wq,
    wo,
    wp,
    tok,
    kv,
    send,
    recv,
    queries,
    gates,
    total,
    heads_all,
    ask_send,
    ask_recv,
    ask_load,
    kv_load,
    load_sem,
    store_sem,
    own_sem,
    tok_far_send,
    tok_far_recv,
    tok_sib_send,
    tok_sib_recv,
    tok_fwd_send,
    tok_fwd_recv,
    kv_send,
    kv_recv,
    ho_far_send,
    ho_far_recv,
    ho_sib_send,
    ho_sib_recv,
    ho_fwd_send,
    ho_fwd_recv,
):
    st = lax.axis_index("st")
    tp = lax.axis_index("tp")
    rows = tokens_hbm.shape[0]
    width = tokens_hbm.shape[1]
    full = width * n_tp
    n_head = queries.shape[0]
    n_pass, plen = kv.shape[1], kv.shape[2]
    chunks = rows // SEQ_LEN
    fars = list(range(2, n_tp, 2))
    st_masks = list(range(n_st - 1, 0, -1))
    sib = flip(tp, 1)

    loads = [
        pltpu.make_async_copy(src, dst, load_sem.at[i])
        for i, (src, dst) in enumerate(
            [
                (query_weight_hbm, wq),
                (out_weight_hbm, wo),
                (pool_weight_hbm.at[0], wp),
            ]
        )
    ]
    per_step = SEQ_LEN // plen
    steps = n_pass // per_step

    def store_load(i):
        part = pl.ds(i * per_step, per_step)
        return pltpu.make_async_copy(store_hbm.at[part], store.at[part], store_sem.at[i])

    def kv_weight_load(h, side):
        source = (key_weight_hbm, value_weight_hbm)[side]
        return pltpu.make_async_copy(
            source.at[:, pl.ds(h * HD, HD)],
            wkv.at[h, :, pl.ds(side * HD, HD)],
            kv_load.at[h, side],
        )

    store_load(0).start()
    for side in range(2):
        kv_weight_load(0, side).start()
    for i in range(1, steps):
        store_load(i).start()
    for h in range(1, n_head):
        for side in range(2):
            kv_weight_load(h, side).start()
    own_load = pltpu.make_async_copy(tokens_hbm, tok.at[tp], own_sem)
    own_load.start()
    for load in loads:
        load.start()

    barrier = pltpu.get_barrier_semaphore()
    peers = [{"tp": sib}] + [{"tp": flip(tp, m)} for m in fars]
    peers += [{"st": flip(st, m)} for m in st_masks]
    for peer in peers:
        pl.semaphore_signal(barrier, inc=1, device_id=peer, device_id_type=MESH)
    pl.semaphore_wait(barrier, len(peers))

    def remote(src, dst, send_sem, recv_sem, peer):
        return pltpu.make_async_remote_copy(
            src_ref=src,
            dst_ref=dst,
            send_sem=send_sem,
            recv_sem=recv_sem,
            device_id=peer,
            device_id_type=MESH,
        )

    def ask(j):
        peer = flip(st, st_masks[j])
        return remote(
            table_ref.at[peer], asked_in.at[st], ask_send.at[j], ask_recv.at[j], {"st": peer}
        )

    for j in range(len(st_masks)):
        ask(j).start()

    def chunk_rows(r):
        return pl.ds(pl.multiple_of(r * SEQ_LEN, SEQ_LEN), SEQ_LEN)

    def tok_far(i, r):
        return remote(
            tokens_hbm.at[chunk_rows(r)],
            tok.at[tp, chunk_rows(r)],
            tok_far_send.at[i, r],
            tok_far_recv.at[i, r],
            {"tp": flip(tp, fars[i])},
        )

    def tok_sib(r):
        return remote(
            tokens_hbm.at[chunk_rows(r)],
            tok.at[tp, chunk_rows(r)],
            tok_sib_send.at[r],
            tok_sib_recv.at[r],
            {"tp": sib},
        )

    def tok_fwd(i, r):
        ref = tok.at[flip(tp, fars[i]), chunk_rows(r)]
        return remote(ref, ref, tok_fwd_send.at[i, r], tok_fwd_recv.at[i, r], {"tp": sib})

    for r in range(chunks):
        for i in range(len(fars)):
            tok_far(i, r).start()
    for r in range(chunks):
        tok_sib(r).start()

    def project(h):
        def step(i, carry):
            part = pl.ds(i * per_step, per_step)
            if h == 0:
                store_load(i).wait()
                x = store[part].reshape(SEQ_LEN, full)
                wide = x.astype(jnp.float32)
                inverse = lax.rsqrt(jnp.sum(wide * wide, axis=1, keepdims=True) / full + epsilon)
                normed = (wide * inverse * passage_gain_ref[...]).astype(jnp.bfloat16)
                store[part] = normed.reshape(per_step, plen, full)
            else:
                normed = store[part].reshape(SEQ_LEN, full)
            both = jnp.dot(normed, wkv[h], preferred_element_type=jnp.float32)
            kv[h, part] = both.astype(jnp.bfloat16).reshape(per_step, plen, 2 * HD)
            return carry

        for side in range(2):
            kv_weight_load(h, side).wait()
        lax.fori_loop(0, steps, step, 0)

    def kv_copy(h, j):
        return remote(
            send.at[h, j],
            recv[h].at[pl.ds(st * cap, cap)],
            kv_send.at[h, j],
            kv_recv.at[h, j],
            {"st": flip(st, st_masks[j])},
        )

    def asked_load(j):
        if j == len(st_masks):
            return pltpu.make_async_copy(table_ref.at[st], asked.at[st], ask_load.at[j])
        peer = flip(st, st_masks[j])
        return pltpu.make_async_copy(asked_in.at[peer], asked.at[peer], ask_load.at[j])

    for h in range(n_head):
        project(h)
        if h == 0:
            for j in range(len(st_masks)):
                ask(j).wait_recv()
                asked_load(j).start()
            asked_load(len(st_masks)).start()
            for j in range(len(st_masks) + 1):
                asked_load(j).wait()
        for j, mask in enumerate(st_masks):
            peer = flip(st, mask)
            for c in range(cap):
                send[h, j, c] = kv[h, asked[peer, 0, c]]
            kv_copy(h, j).start()
    for h in range(n_head):
        for c in range(cap):
            recv[h][st * cap + c] = kv[h, asked[st, 0, c]]

    own_load.wait()
    for load in loads:
        load.wait()
    window_step = tp

    def token_step(r, carry):
        for i in range(len(fars)):
            tok_far(i, r).wait_recv()
            tok_fwd(i, r).start()
        tok_sib(r).wait_recv()
        for i in range(len(fars)):
            tok_fwd(i, r).wait_recv()
        here = chunk_rows(r)
        squares = jnp.zeros((SEQ_LEN, 1), jnp.float32)
        for j in range(n_tp):
            wide = tok[j, here, :].astype(jnp.float32)
            squares = squares + jnp.sum(wide * wide, axis=1, keepdims=True)
        inverse = lax.rsqrt(squares / full + epsilon)
        query = jnp.zeros((SEQ_LEN, n_head * HD), jnp.float32)
        gate = jnp.zeros((SEQ_LEN, gate_weight_ref.shape[0]), jnp.float32)
        for j in range(n_tp):
            cols = pl.ds(j * width, width)
            wide = tok[j, here, :].astype(jnp.float32)
            normed = (wide * inverse * norm_gain_ref[:, cols]).astype(jnp.bfloat16)
            query = query + jnp.dot(normed, wq[cols, :], preferred_element_type=jnp.float32)
            gate = gate + lax.dot_general(
                normed,
                gate_weight_ref[:, cols],
                (((1,), (1,)), ((), ())),
                preferred_element_type=jnp.float32,
            )
        query = query.astype(jnp.bfloat16)
        gate = jax.nn.sigmoid(gate)
        lane = lax.broadcasted_iota(jnp.int32, gate.shape, 1)
        for h in range(n_head):
            queries[h, here, :] = query[:, h * HD : (h + 1) * HD]
            column = jnp.sum(
                jnp.where(lane == tp * n_head + h, gate, 0.0), axis=1, keepdims=True
            )
            gates[h, here, :] = jnp.broadcast_to(column, (SEQ_LEN, HD))
        own_cols = pl.ds(pl.multiple_of(tp * width, width), width)
        wide = tok[tp, here, :].astype(jnp.float32)
        mine = (wide * inverse * norm_gain_ref[:, own_cols]).astype(jnp.bfloat16)
        mine = mine.astype(jnp.float32)
        position = lax.broadcasted_iota(jnp.int32, (SEQ_LEN, width), 0)
        summed = mine
        for level in range(n_tp):
            shift = 2**level
            moved = jnp.where(position >= shift, pltpu.roll(summed, shift, axis=0), 0.0)
            summed = jnp.where(window_step >= level, summed + moved, summed)
        window = jnp.int32(2)
        for level in range(1, n_tp):
            window = jnp.where(window_step >= level, jnp.int32(2 ** (level + 1)), window)
        divisor = jnp.minimum(position + 1, window).astype(jnp.float32)
        pooled = (summed / divisor - mine).astype(jnp.bfloat16)
        mixing = jnp.dot(pooled, wp[...], preferred_element_type=jnp.float32)
        total[here, :] = mixing * pool_scale_ref[...]
        return carry

    lax.fori_loop(0, chunks, token_step, 0)

    def ho_far(h, i, r):
        ref = heads_all.at[h, tp, chunk_rows(r)]
        return remote(
            ref,
            ref,
            ho_far_send.at[h, i, r],
            ho_far_recv.at[h, i, r],
            {"tp": flip(tp, fars[i])},
        )

    def ho_sib(h, r):
        ref = heads_all.at[h, tp, chunk_rows(r)]
        return remote(ref, ref, ho_sib_send.at[h, r], ho_sib_recv.at[h, r], {"tp": sib})

    def ho_fwd(h, i, r):
        ref = heads_all.at[h, flip(tp, fars[i]), chunk_rows(r)]
        return remote(
            ref, ref, ho_fwd_send.at[h, i, r], ho_fwd_recv.at[h, i, r], {"tp": sib}
        )

    blocks = SEQ_LEN // BLK
    scale = HD ** (-0.5)

    for h in range(n_head):
        for j in range(len(st_masks)):
            kv_copy(h, j).wait_recv()

        def attend(r, carry, h=h):
            for inner in range(blocks):
                block = r * blocks + inner
                here = pl.ds(pl.multiple_of(block * BLK, BLK), BLK)
                pieces = [recv[h][place_ref[block * NPB + n]] for n in range(NPB)]
                keys = jnp.concatenate([p[:, :HD] for p in pieces], axis=0)
                vals = jnp.concatenate([p[:, HD:] for p in pieces], axis=0)
                scores = (
                    lax.dot_general(
                        queries[h, here, :],
                        keys,
                        (((1,), (1,)), ((), ())),
                        preferred_element_type=jnp.float32,
                    )
                    * scale
                )
                weights = jnp.exp(scores - jnp.max(scores, axis=1, keepdims=True))
                probs = weights / jnp.sum(weights, axis=1, keepdims=True)
                attended = jnp.dot(
                    probs.astype(jnp.bfloat16), vals, preferred_element_type=jnp.float32
                )
                heads_all[h, tp, here, :] = (attended * gates[h, here, :]).astype(jnp.bfloat16)
            for i in range(len(fars)):
                ho_far(h, i, r).start()
            ho_sib(h, r).start()
            return carry

        lax.fori_loop(0, chunks, attend, 0)

        def forward(r, carry, h=h):
            for i in range(len(fars)):
                ho_far(h, i, r).wait_recv()
                ho_fwd(h, i, r).start()
            return carry

        def finish(r, carry, h=h):
            ho_sib(h, r).wait_recv()
            for i in range(len(fars)):
                ho_fwd(h, i, r).wait_recv()
            here = chunk_rows(r)
            acc = total[here, :]
            for j in range(n_tp):
                acc = acc + jnp.dot(
                    heads_all[h, j, here, :],
                    wo[pl.ds((j * n_head + h) * HD, HD), :],
                    preferred_element_type=jnp.float32,
                )
            if h == n_head - 1:
                out_ref[here, :] = acc.astype(out_ref.dtype)
            else:
                total[here, :] = acc
            return carry

        lax.fori_loop(0, chunks, forward, 0)
        lax.fori_loop(0, chunks, finish, 0)

    def drain(r, carry):
        for i in range(len(fars)):
            tok_far(i, r).wait_send()
            tok_fwd(i, r).wait_send()
        tok_sib(r).wait_send()
        for h in range(n_head):
            for i in range(len(fars)):
                ho_far(h, i, r).wait_send()
                ho_fwd(h, i, r).wait_send()
            ho_sib(h, r).wait_send()
        return carry

    lax.fori_loop(0, chunks, drain, 0)
    for j in range(len(st_masks)):
        ask(j).wait_send()
    for h in range(n_head):
        for j in range(len(st_masks)):
            kv_copy(h, j).wait_send()


def per_device(
    tokens,
    norm_gain,
    pool_weight,
    pool_scale,
    query_weight,
    gate_weight,
    key_weight,
    value_weight,
    out_weight,
    passage_gain,
    passage_store,
    passage_ids,
):
    n_st = lax.axis_size("st")
    n_tp = lax.axis_size("tp")
    rows, width = tokens.shape
    full = width * n_tp
    n_head = query_weight.shape[1] // HD
    n_pass, plen = passage_store.shape[:2]
    chunks = rows // SEQ_LEN
    nf = max(1, (n_tp - 1) // 2)

    flat_ids = passage_ids.reshape(-1)
    asked_count = flat_ids.shape[0]
    cap = max(2, (asked_count + n_st - 1) // n_st)
    owners = lax.div(flat_ids, jnp.int32(n_pass))
    local_index = lax.rem(flat_ids, jnp.int32(n_pass))
    order_index = jnp.arange(asked_count, dtype=jnp.int32)
    earlier = (owners[None, :] == owners[:, None]) & (order_index[None, :] < order_index[:, None])
    slot_index = jnp.sum(earlier.astype(jnp.int32), axis=1)
    place = owners * cap + slot_index
    lanes = jnp.arange(LANES, dtype=jnp.int32)
    owner_range = jnp.arange(n_st, dtype=jnp.int32)
    hit = (owners[None, None, None, :] == owner_range[:, None, None, None]) & (
        slot_index[None, None, None, :] == lanes[None, None, :, None]
    )
    table = jnp.sum(jnp.where(hit, local_index[None, None, None, :], 0), axis=3)

    any_spec = pl.BlockSpec(memory_space=pl.ANY)
    vmem = pl.BlockSpec(memory_space=pltpu.VMEM)
    smem = pl.BlockSpec(memory_space=pltpu.SMEM)
    bf = jnp.bfloat16
    dma = pltpu.SemaphoreType.DMA
    return pl.pallas_call(
        functools.partial(mixer_kernel, n_st, n_tp, cap),
        out_shape=jax.ShapeDtypeStruct((rows, width), bf),
        in_specs=[
            vmem,
            smem,
            any_spec,
            vmem,
            any_spec,
            vmem,
            any_spec,
            vmem,
            any_spec,
            any_spec,
            any_spec,
            vmem,
            any_spec,
        ],
        out_specs=vmem,
        scratch_shapes=[
            pltpu.VMEM((n_st, 1, LANES), jnp.int32),
            pltpu.SMEM((n_st, 1, LANES), jnp.int32),
            pltpu.VMEM(passage_store.shape, bf),
            pltpu.VMEM((n_head, full, 2 * HD), bf),
            pltpu.VMEM(query_weight.shape, bf),
            pltpu.VMEM(out_weight.shape, bf),
            pltpu.VMEM(pool_weight.shape[1:], bf),
            pltpu.VMEM((n_tp, rows, width), bf),
            pltpu.VMEM((n_head, n_pass, plen, 2 * HD), bf),
            pltpu.VMEM((n_head, n_st - 1, cap, plen, 2 * HD), bf),
            [pltpu.VMEM((n_st * cap, plen, 2 * HD), bf) for _ in range(n_head)],
            pltpu.VMEM((n_head, rows, HD), bf),
            pltpu.VMEM((n_head, rows, HD), jnp.float32),
            pltpu.VMEM((rows, width), jnp.float32),
            pltpu.VMEM((n_head, n_tp, rows, HD), bf),
            dma((n_st - 1,)),
            dma((n_st - 1,)),
            dma((n_st,)),
            dma((n_head, 2)),
            dma((3,)),
            dma((n_pass * plen // SEQ_LEN,)),
            dma,
            dma((nf, chunks)),
            dma((nf, chunks)),
            dma((chunks,)),
            dma((chunks,)),
            dma((nf, chunks)),
            dma((nf, chunks)),
            dma((n_head, n_st - 1)),
            dma((n_head, n_st - 1)),
            dma((n_head, nf, chunks)),
            dma((n_head, nf, chunks)),
            dma((n_head, chunks)),
            dma((n_head, chunks)),
            dma((n_head, nf, chunks)),
            dma((n_head, nf, chunks)),
        ],
        compiler_params=pltpu.CompilerParams(
            collective_id=0, has_side_effects=True, vmem_limit_bytes=60 * 1024 * 1024
        ),
        name="mixer",
    )(
        table,
        place,
        tokens,
        norm_gain.reshape(1, full),
        pool_weight,
        pool_scale.reshape(1, width),
        query_weight,
        gate_weight.T,
        key_weight,
        value_weight,
        out_weight,
        passage_gain.reshape(1, full),
        passage_store,
    )


def solution(mesh):
    in_specs = (
        P(("grp", "st"), "tp"),
        P(),
        P("tp", None, None),
        P("tp"),
        P(None, "tp"),
        P(),
        P(None, "tp"),
        P(None, "tp"),
        P(None, "tp"),
        P(),
        P(("grp", "st"), None, None),
        P(("grp", "st"), None),
    )
    out_specs = P(("grp", "st"), "tp")
    return jax.shard_map(
        per_device, mesh=mesh, in_specs=in_specs, out_specs=out_specs, check_vma=False
    )
```
